32 devices in a mesh: rep: 4 (over z), fs: 4 (over y, x), tp: 2 (over core).
Axes of the slice: x: 2, y: 2, z: 4, core: 2. Of those that a mesh axis runs over, the one named last changes fastest.
Arguments:
- pre_gate: bfloat16 [3072, 7936], P('rep', ('fs', 'tp')), may hold values from -6 to 6
- pre_up: bfloat16 [3072, 7936], P('rep', ('fs', 'tp')), may hold values from -6 to 6
- cotangent: bfloat16 [3072, 4096], P('rep', ('fs', 'tp')), may hold values from -6 to 6
- down_weight: bfloat16 [7936, 4096], P(('fs', 'tp')), may hold values from -0.0625 to 0.0625
Outputs:
- grad_gate: bfloat16 [3072, 7936], P('rep', ('fs', 'tp'))
- grad_up: bfloat16 [3072, 7936], P('rep', ('fs', 'tp'))
- grad_down: float32 [7936, 4096], P(('fs', 'tp'), 'rep')
- row_squares: float32 [7936], P(('fs', 'tp'))
The draws below stay inside these ranges and needn't reach their ends.
All inputs are finite; a program needn't handle non-finite values.
Results may differ from the reference program's by a relative error of at most 0.0034.
Values may be sent and summed in bfloat16 or wider, within the bound.
A program may use at most 128 MiB of HBM per device.

```python
import jax
import jax.numpy as jnp

D = 4096
FF = 7936
TOKENS = 3072


def with_spikes(result, rng, source, target, shards_of, factor):
    def block_of(axis_at):
        return (jnp.arange(result.shape[axis_at]) // (result.shape[axis_at] // shards_of)).reshape((-1,) + (1,) * (result.ndim - 1 - axis_at))

    first = jax.random.permutation(rng, shards_of)[block_of(target)]
    other_side = (block_of(target) + shards_of // 2) % shards_of
    return jnp.where((block_of(source) == first) | (block_of(source) == other_side), factor * result, result)


def level_of(rng, extent, shards, low, top_value):
    def one(dim, blocks):
        steps = jax.random.uniform(jax.random.fold_in(jax.random.fold_in(rng, 6), dim), (blocks,), jnp.float32, low / len(shards), top_value / len(shards))
        return jnp.repeat(jnp.exp(steps), extent[dim] // blocks).reshape((-1,) + (1,) * (len(extent) - dim - 1))

    gain = one(*shards[0])
    for cut in shards[1:]:
        gain = gain * one(*cut)
    return gain


def normal_values(own_key, dims, scale, reach, shards=(), dtype=jnp.bfloat16):
    entries = scale * jax.random.normal(own_key, dims, jnp.float32)
    if shards:
        entries = entries * level_of(own_key, dims, shards, -0.22, 0.18)
    return jnp.clip(entries, -reach, reach).astype(dtype)


def bell_draw_with(stream_key, dims, spread, most, cuts, heavy, held_as=jnp.bfloat16):
    drawn = spread * jax.random.normal(stream_key, dims, jnp.float32)
    if cuts:
        drawn = drawn * level_of(stream_key, dims, cuts, -0.22, 0.18)
    return jnp.clip(with_spikes(drawn, jax.random.fold_in(stream_key, 3), *heavy), -most, most).astype(held_as)


def setup_inputs(seed: int = 0) -> dict:
    arg_keys = jax.random.split(jax.random.key(seed), 5)
    pre_gate = normal_values(arg_keys[0], (TOKENS, FF), 1.5, 6.0, ((0, 4), (1, 8)))
    pre_up = normal_values(arg_keys[1], (TOKENS, FF), 1.0, 6.0, ((0, 4), (1, 8)))
    cotangent = bell_draw_with(arg_keys[2], (TOKENS, D), 1.0, 6.0, ((0, 4), (1, 8)), (0, 1, 8, 2.0))
    down_weight = normal_values(arg_keys[3], (FF, D), FF ** -0.5, 0.0625, ((0, 8),))
    return dict(pre_gate=pre_gate, pre_up=pre_up, cotangent=cotangent, down_weight=down_weight)


def reference(pre_gate, pre_up, cotangent, down_weight):
    gate_wide = pre_gate.astype(jnp.float32)
    up_wide = pre_up.astype(jnp.float32)
    sigmoid_gate = jax.nn.sigmoid(gate_wide)
    act = gate_wide * sigmoid_gate
    hidden = (act * up_wide).astype(jnp.bfloat16)
    grad_hidden = jnp.dot(cotangent, down_weight.T, preferred_element_type=jnp.float32)
    grad_up = (grad_hidden * act).astype(jnp.bfloat16)
    slope = sigmoid_gate * (1.0 + gate_wide * (1.0 - sigmoid_gate))
    grad_gate = (grad_hidden * up_wide * slope).astype(jnp.bfloat16)
    grad_down = jnp.dot(hidden.T, cotangent, preferred_element_type=jnp.float32)
    row_squares = jnp.sum(grad_down * grad_down, axis=1)
    return grad_gate, grad_up, grad_down, row_squares
```

```python
import jax
import jax.numpy as jnp
from jax import lax
from jax.experimental import pallas as pl
from jax.experimental.pallas import tpu as pltpu
from jax.sharding import PartitionSpec as P

MESH = pl.DeviceIdType.MESH
F32 = jnp.float32
BF16 = jnp.bfloat16


def local(pre_gate, pre_up, cotangent, down_weight):
    gate_wide = pre_gate.astype(F32)
    up_wide = pre_up.astype(F32)
    sigmoid_gate = jax.nn.sigmoid(gate_wide)
    act = gate_wide * sigmoid_gate
    hidden = (act * up_wide).astype(BF16)
    piece = lax.all_gather(cotangent, ("fs", "tp"), axis=1, tiled=True)
    partial_grad = lax.dot_general(
        piece, down_weight, (((1,), (1,)), ((), ())), preferred_element_type=F32
    )
    block = lax.dot_general(
        piece, hidden, (((0,), (0,)), ((), ())), preferred_element_type=F32
    )
    grad_up = (partial_grad * act).astype(BF16)
    slope = sigmoid_gate * (1.0 + gate_wide * (1.0 - sigmoid_gate))
    grad_gate = (partial_grad * up_wide * slope).astype(BF16)
    shard_rows = lax.psum_scatter(block, "rep", scatter_dimension=0, tiled=True)
    grad_down = shard_rows.T
    row_squares = lax.psum(jnp.sum(grad_down * grad_down, axis=1), "rep")
    return (grad_gate, grad_up, grad_down, row_squares)


CHUNKS = 4
OWN, G0, G1, G2 = 0, 7, 14, 21
ZX0, ZX1, ZY, ZF = 28, 29, 31, 33
HO_S = 34
HM_S = HO_S + CHUNKS
HF_S = HM_S + CHUNKS
C_S = HF_S + CHUNKS
N_SEM = C_S + CHUNKS


def chunk_rows(rows):
    step = -(-rows // CHUNKS)
    step = -(-step // 16) * 16
    return [(a, min(step, rows - a)) for a in range(0, rows, step)]


def kernel(gate, up, shard, w, hid, gg, gu, out,
           G, X, Y, HO, HM, HF, CS, CR, ssem, rsem):
    rep = lax.axis_index("rep")
    fs = lax.axis_index("fs")
    tp = lax.axis_index("tp")
    tokens, wide = shard.shape
    rows = hid.shape[0]
    cols = out.shape[1]
    sub = Y.shape[2]
    x, y = fs % 2, fs // 2
    peers = (y * 2 + (1 - x), (1 - y) * 2 + x, (1 - y) * 2 + (1 - x))
    me = fs * 2 + tp
    side = rep // 2
    inner = (rep == 1) | (rep == 2)
    outer = (rep == 0) | (rep == 3)
    mid = 3 - rep
    edge = side * 3
    inn = 1 + side
    other = 1 - side
    partner = (rep, fs, 1 - tp)
    parts = chunk_rows(rows)

    def copy(src, dst, i, dev):
        return pltpu.make_async_remote_copy(
            src_ref=src, dst_ref=dst, send_sem=ssem.at[i], recv_sem=rsem.at[i],
            device_id=dev, device_id_type=MESH)

    def at(start, size):
        return pl.ds(pl.multiple_of(start, 128), size)

    barrier = pltpu.get_barrier_semaphore()

    def hello(dev):
        pl.semaphore_signal(barrier, inc=1, device_id=dev, device_id_type=MESH)

    for q in peers:
        hello((rep, q, tp))
    hello(partner)

    @pl.when(outer)
    def _():
        hello((inn, fs, tp))
        pl.semaphore_wait(barrier, 5)

    @pl.when(inner)
    def _():
        hello((mid, fs, tp))
        hello((edge, fs, tp))
        pl.semaphore_wait(barrier, 6)

    def send_plane(base, src, view):
        for k, q in enumerate(peers):
            copy(src, view(me), base + k, (rep, q, tp)).start()
        copy(src, view(me), base + 3, partner).start()

    def relay_plane(base, view):
        for k, q in enumerate(peers):
            v = view(q * 2 + tp)
            copy(v, v, base + k, partner).wait_recv()
            copy(v, v, base + 4 + k, partner).start()

    def finish_plane(base, view):
        v = view(fs * 2 + 1 - tp)
        copy(v, v, base + 3, partner).wait_recv()
        for k, q in enumerate(peers):
            v = view(q * 2 + 1 - tp)
            copy(v, v, base + 4 + k, partner).wait_recv()

    def sent_plane(base, view):
        for k in range(7):
            copy(view(me), view(me), base + k, partner).wait_send()

    def own_view(p):
        return G.at[:, at(p * wide, wide)]

    def x_view(u, n):
        return lambda p: X.at[pl.ds(u, n), :, at(p * sub, sub)]

    def unit(u):
        return X.at[u, :, at(me * sub, sub)]

    def gcol(c):
        return G.at[:, at(c * cols + me * sub, sub)]

    v0, v1, v2 = x_view(0, 1), x_view(1, 2), x_view(3, 2)

    send_plane(OWN, shard, own_view)

    @pl.when(outer)
    def _():
        for c, (a, n) in enumerate(parts):
            copy(hid.at[pl.ds(a, n)], HO.at[pl.ds(a, n)], HO_S + c, (inn, fs, tp)).start()

    @pl.when(inner)
    def _():
        for c, (a, n) in enumerate(parts):
            copy(hid.at[pl.ds(a, n)], HM.at[pl.ds(a, n)], HM_S + c, (mid, fs, tp)).start()

    G[:, at(me * wide, wide)] = shard[...]
    relay_plane(OWN, own_view)
    finish_plane(OWN, own_view)

    def hidden_grads():
        tile = 256

        @pl.loop(0, tokens // tile)
        def _(t):
            r = pl.ds(pl.multiple_of(t * tile, tile), tile)
            pg = lax.dot_general(G[r, :], w[...], (((1,), (1,)), ((), ())),
                                 preferred_element_type=F32)
            g = gate[r, :].astype(F32)
            u = up[r, :].astype(F32)
            s = 1.0 / (1.0 + jnp.exp(-g))
            gu[r, :] = (pg * (g * s)).astype(BF16)
            gg[r, :] = (pg * u * (s * (1.0 + g * (1.0 - s)))).astype(BF16)

    def dot(h, a, n, b):
        return jnp.dot(h[pl.ds(a, n), :], b, preferred_element_type=F32)

    @pl.when(outer)
    def _():
        to = (inn, fs, tp)
        for j in range(2):
            copy(gcol(other * 2 + j), Y.at[j], ZY + j, to).start()
        copy(gcol(inn), unit(0), ZX0, to).start()
        hidden_grads()
        for c, (a, n) in enumerate(parts):
            out[pl.ds(a, n), :] = dot(hid, a, n, G[:, at(rep * cols, cols)])
        for c, (a, n) in enumerate(parts):
            r = pl.ds(a, n)
            copy(CS.at[r], CR.at[r], C_S + c, to).wait_recv()
            out[r, :] = out[r, :] + CR[r, :].astype(F32)
        for c, (a, n) in enumerate(parts):
            copy(hid.at[pl.ds(a, n)], HO.at[pl.ds(a, n)], HO_S + c, to).wait_send()
        for j in range(2):
            copy(Y.at[j], Y.at[j], ZY + j, to).wait_send()
        copy(unit(0), unit(0), ZX0, to).wait_send()

    @pl.when(inner)
    def _():
        to = (mid, fs, tp)
        back = (edge, fs, tp)
        for j in range(2):
            copy(gcol(other * 2 + j), unit(1 + j), ZX1 + j, to).start()

        def forward(c):
            a, n = parts[c]
            v = HO.at[pl.ds(a, n)]
            copy(v, v, HO_S + c, to).wait_recv()
            copy(v, HF.at[pl.ds(a, n)], HF_S + c, to).start()

        forward(0)
        for j in range(2):
            copy(Y.at[j], Y.at[j], ZY + j, to).wait_recv()
        copy(Y, v2(me), ZF, to).start()
        for c in range(1, len(parts)):
            forward(c)
        for j in range(2):
            copy(unit(1 + j), unit(1 + j), ZX1 + j, to).wait_recv()
        send_plane(G1, v1(me), v1)
        copy(unit(0), unit(0), ZX0, to).wait_recv()
        send_plane(G0, v0(me), v0)
        relay_plane(G1, v1)
        relay_plane(G0, v0)
        hidden_grads()
        copy(v2(me), v2(me), ZF, to).wait_recv()
        send_plane(G2, v2(me), v2)
        finish_plane(G1, v1)
        finish_plane(G0, v0)
        relay_plane(G2, v2)
        finish_plane(G2, v2)
        jr = rep % 2
        je = 1 - jr
        for c, (a, n) in enumerate(parts):
            r = pl.ds(a, n)
            copy(HM.at[r], HM.at[r], HM_S + c, to).wait_recv()
            copy(HF.at[r], HF.at[r], HF_S + c, to).wait_recv()
            total = dot(hid, a, n, G[:, at(edge * cols, cols)])
            total = total + dot(HM, a, n, X[1 + je])
            total = total + dot(HF, a, n, X[3 + je])
            CS[r, :] = total.astype(BF16)
            copy(CS.at[r], CR.at[r], C_S + c, back).start()
        for c, (a, n) in enumerate(parts):
            total = dot(hid, a, n, G[:, at(rep * cols, cols)])
            total = total + dot(HO, a, n, X[0])
            total = total + dot(HM, a, n, X[1 + jr])
            total = total + dot(HF, a, n, X[3 + jr])
            out[pl.ds(a, n), :] = total
        for j in range(2):
            copy(unit(1 + j), unit(1 + j), ZX1 + j, to).wait_send()
        copy(Y, v2(me), ZF, to).wait_send()
        for c, (a, n) in enumerate(parts):
            r = pl.ds(a, n)
            copy(HM.at[r], HM.at[r], HM_S + c, to).wait_send()
            copy(HF.at[r], HF.at[r], HF_S + c, to).wait_send()
            copy(CS.at[r], CS.at[r], C_S + c, back).wait_send()
        sent_plane(G0, v0)
        sent_plane(G1, v1)
        sent_plane(G2, v2)

    sent_plane(OWN, own_view)


def fused(pre_gate, pre_up, cotangent, down_weight):
    tokens, rows = pre_gate.shape
    width = down_weight.shape[1]
    reps = lax.axis_size("rep")
    plane = width // cotangent.shape[1]
    cols = width // reps
    g = pre_gate.astype(F32)
    hid = (g * jax.nn.sigmoid(g) * pre_up.astype(F32)).astype(BF16).T
    vmem = pl.BlockSpec(memory_space=pltpu.VMEM)
    hid_buf = pltpu.VMEM((rows, tokens), BF16)
    gg, gu, out = pl.pallas_call(
        kernel,
        out_shape=(
            jax.ShapeDtypeStruct((tokens, rows), BF16),
            jax.ShapeDtypeStruct((tokens, rows), BF16),
            jax.ShapeDtypeStruct((rows, cols), F32),
        ),
        in_specs=[vmem] * 5,
        out_specs=(vmem,) * 3,
        scratch_shapes=[
            pltpu.VMEM((tokens, width), BF16),
            pltpu.VMEM((5, tokens, cols), BF16),
            pltpu.VMEM((2, tokens, cols // plane), BF16),
            hid_buf, hid_buf, hid_buf,
            pltpu.VMEM((rows, cols), BF16),
            pltpu.VMEM((rows, cols), BF16),
            pltpu.SemaphoreType.DMA((N_SEM,)),
            pltpu.SemaphoreType.DMA((N_SEM,)),
        ],
        compiler_params=pltpu.CompilerParams(
            collective_id=0, has_side_effects=True, vmem_limit_bytes=67043328),
    )(pre_gate, pre_up, cotangent, down_weight, hid)
    row_squares = lax.psum(jnp.sum(out * out, axis=1), "rep")
    return gg, gu, out, row_squares


def solution(mesh):
    placed = (
        P("rep", ("fs", "tp")),
        P("rep", ("fs", "tp")),
        P("rep", ("fs", "tp")),
        P(("fs", "tp"), None),
    )
    shape = dict(mesh.shape)
    fits = shape["rep"] // 2 == 2 and shape["fs"] // 2 == 2 and shape["tp"] == 2
    return jax.shard_map(
        fused if fits else local,
        mesh=mesh,
        in_specs=placed,
        out_specs=(
            P("rep", ("fs", "tp")),
            P("rep", ("fs", "tp")),
            P(("fs", "tp"), "rep"),
            P(("fs", "tp")),
        ),
        check_vma=False,
    )
```

```python
import jax
import jax.numpy as jnp
from jax import lax
from jax.experimental import pallas as pl
from jax.experimental.pallas import tpu as pltpu
from jax.sharding import PartitionSpec as P

MESH = pl.DeviceIdType.MESH
F32 = jnp.float32
BF16 = jnp.bfloat16


def local(pre_gate, pre_up, cotangent, down_weight):
    gate_wide = pre_gate.astype(F32)
    up_wide = pre_up.astype(F32)
    sigmoid_gate = jax.nn.sigmoid(gate_wide)
    act = gate_wide * sigmoid_gate
    hidden = (act * up_wide).astype(BF16)
    piece = lax.all_gather(cotangent, ("fs", "tp"), axis=1, tiled=True)
    partial_grad = lax.dot_general(
        piece, down_weight, (((1,), (1,)), ((), ())), preferred_element_type=F32
    )
    block = lax.dot_general(
        piece, hidden, (((0,), (0,)), ((), ())), preferred_element_type=F32
    )
    grad_up = (partial_grad * act).astype(BF16)
    slope = sigmoid_gate * (1.0 + gate_wide * (1.0 - sigmoid_gate))
    grad_gate = (partial_grad * up_wide * slope).astype(BF16)
    shard_rows = lax.psum_scatter(block, "rep", scatter_dimension=0, tiled=True)
    grad_down = shard_rows.T
    row_squares = lax.psum(jnp.sum(grad_down * grad_down, axis=1), "rep")
    return (grad_gate, grad_up, grad_down, row_squares)


CHUNKS = 4
OWN, G0, G1E, G1R, G2E, G2R = (8 * i for i in range(6))
ZX, ZM, ZY, ZF, SQ_S = 48, 49, 51, 53, 55
HO_S = 58
HM_S = HO_S + CHUNKS
HF_S = HM_S + CHUNKS
C_S = HF_S + CHUNKS
N_SEM = C_S + CHUNKS


def chunk_rows(rows):
    step = -(-rows // CHUNKS)
    step = -(-step // 16) * 16
    return [(a, min(step, rows - a)) for a in range(0, rows, step)]


def kernel(gate_in, up_in, shard, w_in, hid, gg_out, gu_out, out_out, sq_out,
           G, X, Y, HO, HM, HF, CS, CR, gate, up, w, gg, gu, out, acc, SQ,
           ssem, rsem, lsem):
    rep = lax.axis_index("rep")
    fs = lax.axis_index("fs")
    tp = lax.axis_index("tp")
    tokens, wide = shard.shape
    rows = hid.shape[0]
    cols = out.shape[1]
    sub = Y.shape[2]
    half = tokens // 2
    x, y = fs % 2, fs // 2
    xq, yq, dq = y * 2 + (1 - x), (1 - y) * 2 + x, (1 - y) * 2 + (1 - x)
    me = fs * 2 + tp
    side = rep // 2
    inner = (rep == 1) | (rep == 2)
    outer = (rep == 0) | (rep == 3)
    mid = 3 - rep
    edge = side * 3
    inn = 1 + side
    far_edge = (1 - side) * 3
    far_inn = 2 - side
    partner = (rep, fs, 1 - tp)
    parts = chunk_rows(rows)
    early = range(len(parts) - 1)
    last = len(parts) - 1

    def copy(src, dst, i, dev):
        return pltpu.make_async_remote_copy(
            src_ref=src, dst_ref=dst, send_sem=ssem.at[i], recv_sem=rsem.at[i],
            device_id=dev, device_id_type=MESH)

    def at(start, size):
        return pl.ds(pl.multiple_of(start, 128), size)

    loads = [pltpu.make_async_copy(a, b, lsem.at[i])
             for i, (a, b) in enumerate([(gate_in, gate), (up_in, up), (w_in, w)])]
    for load in loads:
        load.start()

    barrier = pltpu.get_barrier_semaphore()

    def hello(dev):
        pl.semaphore_signal(barrier, inc=1, device_id=dev, device_id_type=MESH)

    for d in range(1, 4):
        hello(((rep + d) % 4, fs, tp))
    for q in (xq, yq):
        hello((rep, q, tp))
    hello(partner)
    pl.semaphore_wait(barrier, 6)

    def send_plane(base, src, view):
        copy(src, view(me), base, (rep, xq, tp)).start()
        copy(src, view(me), base + 1, (rep, yq, tp)).start()
        copy(src, view(me), base + 4, partner).start()

    def top(v):
        return v.at[pl.ds(0, half)]

    def low(v):
        return v.at[pl.ds(half, half)]

    def relay_plane(base, view):
        vx, vy, vd = view(xq * 2 + tp), view(yq * 2 + tp), view(dq * 2 + tp)
        copy(vx, vx, base, partner).wait_recv()
        copy(top(vx), top(vx), base + 2, (rep, yq, tp)).start()
        copy(vx, vx, base + 5, partner).start()
        copy(vy, vy, base + 1, partner).wait_recv()
        copy(low(vy), low(vy), base + 3, (rep, xq, tp)).start()
        copy(vy, vy, base + 6, partner).start()
        copy(top(vd), top(vd), base + 2, partner).wait_recv()
        copy(low(vd), low(vd), base + 3, partner).wait_recv()
        copy(vd, vd, base + 7, partner).start()

    def finish_plane(base, view):
        for k, q in ((4, fs), (5, xq), (6, yq), (7, dq)):
            v = view(q * 2 + 1 - tp)
            copy(v, v, base + k, partner).wait_recv()

    def sent_plane(base, view):
        v = view(me)
        for k in range(8):
            u = top(v) if k in (2, 3) else v
            copy(u, u, base + k, partner).wait_send()

    def own_view(p):
        return G.at[:, at(p * wide, wide)]

    def x_view(u):
        return lambda p: X.at[u, :, at(p * sub, sub)]

    def gcol(c):
        return G.at[:, at(c * cols + me * sub, sub)]

    x_o, m_e, m_r, f_e, f_r = (x_view(u) for u in range(5))

    def chunk(ref, c):
        a, n = parts[c]
        return ref.at[pl.ds(a, n)]

    send_plane(OWN, shard, own_view)

    @pl.when(outer)
    def _():
        for c in early:
            copy(chunk(hid, c), chunk(HO, c), HO_S + c, (inn, fs, tp)).start()

    @pl.when(inner)
    def _():
        for c in early:
            copy(chunk(hid, c), chunk(HM, c), HM_S + c, (mid, fs, tp)).start()

    G[:, at(me * wide, wide)] = shard[...]
    relay_plane(OWN, own_view)
    finish_plane(OWN, own_view)

    def hidden_grads():
        for load in loads:
            load.wait()
        tile = rows // 2

        @pl.loop(0, 2)
        def _(t):
            r = pl.ds(pl.multiple_of(t * tile, 16), tile)
            pg = lax.dot_general(w[r, :], G[...], (((1,), (1,)), ((), ())),
                                 preferred_element_type=F32)
            g = gate[r, :].astype(F32)
            u = up[r, :].astype(F32)
            s = 1.0 / (1.0 + jnp.exp(-g))
            gu[r, :] = (pg * (g * s)).astype(BF16)
            gg[r, :] = (pg * u * (s * (1.0 + g * (1.0 - s)))).astype(BF16)

        pltpu.make_async_copy(gg, gg_out, lsem.at[3]).start()
        pltpu.make_async_copy(gu, gu_out, lsem.at[4]).start()

    def dot(h, c, b):
        a, n = parts[c]
        return jnp.dot(h[pl.ds(a, n), :], b, preferred_element_type=F32)

    def store(c, total):
        a, n = parts[c]
        r = pl.ds(a, n)
        out[r, :] = total
        pltpu.make_async_copy(chunk(out, c), chunk(out_out, c), lsem.at[5 + c]).start()
        square = total * total
        lanes = square[:, 0:128]
        for k in range(1, cols // 128):
            lanes = lanes + square[:, k * 128:(k + 1) * 128]
        acc[r, :] = lanes

    acc[...] = jnp.zeros_like(acc)

    @pl.when(outer)
    def _():
        to = (inn, fs, tp)
        copy(gcol(far_edge), Y.at[0], ZY, to).start()
        copy(gcol(far_inn), Y.at[1], ZY + 1, to).start()
        copy(chunk(hid, last), chunk(HO, last), HO_S + last, to).start()
        copy(gcol(inn), x_o(me), ZX, to).start()
        hidden_grads()
        for c in range(len(parts)):
            a, n = parts[c]
            out[pl.ds(a, n), :] = dot(hid, c, G[:, at(rep * cols, cols)])
        for c in range(len(parts)):
            a, n = parts[c]
            copy(chunk(CS, c), chunk(CR, c), C_S + c, to).wait_recv()
            store(c, out[pl.ds(a, n), :] + CR[pl.ds(a, n), :].astype(F32))
        for c in range(len(parts)):
            copy(chunk(hid, c), chunk(HO, c), HO_S + c, to).wait_send()
        for j in range(2):
            copy(Y.at[j], Y.at[j], ZY + j, to).wait_send()
        copy(x_o(me), x_o(me), ZX, to).wait_send()

    @pl.when(inner)
    def _():
        to = (mid, fs, tp)
        back = (edge, fs, tp)

        def forward(c):
            copy(chunk(HO, c), chunk(HO, c), HO_S + c, to).wait_recv()
            copy(chunk(HO, c), chunk(HF, c), HF_S + c, to).start()

        def arrived(view, i):
            copy(view(me), view(me), i, to).wait_recv()

        copy(gcol(far_edge), m_e(me), ZM, to).start()
        copy(Y.at[0], Y.at[0], ZY, to).wait_recv()
        copy(Y.at[0], f_e(me), ZF, to).start()
        forward(0)
        arrived(m_e, ZM)
        send_plane(G1E, m_e(me), m_e)
        for c in early:
            if c:
                forward(c)
        copy(gcol(mid), m_r(me), ZM + 1, to).start()
        arrived(f_e, ZF)
        send_plane(G2E, f_e(me), f_e)
        copy(Y.at[1], Y.at[1], ZY + 1, to).wait_recv()
        copy(Y.at[1], f_r(me), ZF + 1, to).start()
        copy(chunk(hid, last), chunk(HM, last), HM_S + last, to).start()
        relay_plane(G1E, m_e)
        relay_plane(G2E, f_e)
        forward(last)
        arrived(x_o, ZX)
        send_plane(G0, x_o(me), x_o)
        finish_plane(G1E, m_e)
        finish_plane(G2E, f_e)

        def give(c):
            a, n = parts[c]
            copy(chunk(HM, c), chunk(HM, c), HM_S + c, to).wait_recv()
            copy(chunk(HF, c), chunk(HF, c), HF_S + c, to).wait_recv()
            total = dot(hid, c, G[:, at(edge * cols, cols)])
            total = total + dot(HM, c, X[1])
            total = total + dot(HF, c, X[3])
            CS[pl.ds(a, n), :] = total.astype(BF16)
            copy(chunk(CS, c), chunk(CR, c), C_S + c, back).start()

        for c in early:
            give(c)
        relay_plane(G0, x_o)
        arrived(m_r, ZM + 1)
        send_plane(G1R, m_r(me), m_r)
        arrived(f_r, ZF + 1)
        send_plane(G2R, f_r(me), f_r)
        hidden_grads()
        relay_plane(G1R, m_r)
        relay_plane(G2R, f_r)
        give(last)
        finish_plane(G0, x_o)
        finish_plane(G1R, m_r)
        finish_plane(G2R, f_r)
        for c in range(len(parts)):
            total = dot(hid, c, G[:, at(rep * cols, cols)])
            total = total + dot(HO, c, X[0])
            total = total + dot(HM, c, X[2])
            total = total + dot(HF, c, X[4])
            store(c, total)
        for j in range(2):
            copy(Y.at[j], Y.at[j], ZM + j, to).wait_send()
            copy(Y.at[j], Y.at[j], ZF + j, to).wait_send()
        for c in range(len(parts)):
            copy(chunk(HM, c), chunk(HM, c), HM_S + c, to).wait_send()
            copy(chunk(HF, c), chunk(HF, c), HF_S + c, to).wait_send()
            copy(chunk(CS, c), chunk(CS, c), C_S + c, back).wait_send()
        sent_plane(G0, x_o)
        sent_plane(G1E, m_e)
        sent_plane(G1R, m_r)
        sent_plane(G2E, f_e)
        sent_plane(G2R, f_r)

    sums = jnp.sum(acc[...].T, axis=0, keepdims=True)
    SQ[rep] = jnp.broadcast_to(sums, SQ.shape[1:])
    for d in range(1, 4):
        copy(SQ.at[rep], SQ.at[rep], SQ_S + d - 1, ((rep + d) % 4, fs, tp)).start()
    for d in range(1, 4):
        v = SQ.at[(rep + 4 - d) % 4]
        copy(v, v, SQ_S + d - 1, partner).wait_recv()
    sq_out[...] = (SQ[0] + SQ[1]) + (SQ[2] + SQ[3])
    for d in range(1, 4):
        copy(SQ.at[rep], SQ.at[rep], SQ_S + d - 1, partner).wait_send()
    sent_plane(OWN, own_view)
    pltpu.make_async_copy(gg, gg_out, lsem.at[3]).wait()
    pltpu.make_async_copy(gu, gu_out, lsem.at[4]).wait()
    for c in range(len(parts)):
        pltpu.make_async_copy(chunk(out, c), chunk(out_out, c), lsem.at[5 + c]).wait()


def fused(pre_gate, pre_up, cotangent, down_weight):
    tokens, rows = pre_gate.shape
    width = down_weight.shape[1]
    reps = lax.axis_size("rep")
    plane = width // cotangent.shape[1]
    cols = width // reps
    padded = -(-rows // 128) * 128
    gate_t, up_t = pre_gate.T, pre_up.T
    g = gate_t.astype(F32)
    hid = (g * jax.nn.sigmoid(g) * up_t.astype(F32)).astype(BF16)
    vmem = pl.BlockSpec(memory_space=pltpu.VMEM)
    hbm = pl.BlockSpec(memory_space=pl.ANY)
    hid_buf = pltpu.VMEM((rows, tokens), BF16)
    gg, gu, out, squares = pl.pallas_call(
        kernel,
        out_shape=(
            jax.ShapeDtypeStruct((rows, tokens), BF16),
            jax.ShapeDtypeStruct((rows, tokens), BF16),
            jax.ShapeDtypeStruct((rows, cols), F32),
            jax.ShapeDtypeStruct((8, padded), F32),
        ),
        in_specs=[hbm, hbm, vmem, hbm, vmem],
        out_specs=(hbm, hbm, hbm, vmem),
        scratch_shapes=[
            pltpu.VMEM((tokens, width), BF16),
            pltpu.VMEM((5, tokens, cols), BF16),
            pltpu.VMEM((2, tokens, cols // plane), BF16),
            hid_buf, hid_buf, hid_buf,
            pltpu.VMEM((rows, cols), BF16),
            pltpu.VMEM((rows, cols), BF16),
            hid_buf, hid_buf,
            pltpu.VMEM((rows, width), BF16),
            hid_buf, hid_buf,
            pltpu.VMEM((rows, cols), F32),
            pltpu.VMEM((padded, 128), F32),
            pltpu.VMEM((4, 8, padded), F32),
            pltpu.SemaphoreType.DMA((N_SEM,)),
            pltpu.SemaphoreType.DMA((N_SEM,)),
            pltpu.SemaphoreType.DMA((5 + CHUNKS,)),
        ],
        compiler_params=pltpu.CompilerParams(
            collective_id=0, has_side_effects=True, vmem_limit_bytes=67043328),
    )(gate_t, up_t, cotangent, down_weight, hid)
    return gg.T, gu.T, out, squares[0, :rows]


def solution(mesh):
    placed = (
        P("rep", ("fs", "tp")),
        P("rep", ("fs", "tp")),
        P("rep", ("fs", "tp")),
        P(("fs", "tp"), None),
    )
    shape = dict(mesh.shape)
    fits = shape["rep"] // 2 == 2 and shape["fs"] // 2 == 2 and shape["tp"] == 2
    return jax.shard_map(
        fused if fits else local,
        mesh=mesh,
        in_specs=placed,
        out_specs=(
            P("rep", ("fs", "tp")),
            P("rep", ("fs", "tp")),
            P(("fs", "tp"), "rep"),
            P(("fs", "tp")),
        ),
        check_vma=False,
    )
```

```python
import jax
import jax.numpy as jnp
from jax import lax
from jax.experimental import pallas as pl
from jax.experimental.pallas import tpu as pltpu
from jax.sharding import PartitionSpec as P

MESH = pl.DeviceIdType.MESH
F32 = jnp.float32
BF16 = jnp.bfloat16


def local(pre_gate, pre_up, cotangent, down_weight):
    gate_wide = pre_gate.astype(F32)
    up_wide = pre_up.astype(F32)
    sigmoid_gate = jax.nn.sigmoid(gate_wide)
    act = gate_wide * sigmoid_gate
    hidden = (act * up_wide).astype(BF16)
    piece = lax.all_gather(cotangent, ("fs", "tp"), axis=1, tiled=True)
    partial_grad = lax.dot_general(
        piece, down_weight, (((1,), (1,)), ((), ())), preferred_element_type=F32
    )
    block = lax.dot_general(
        piece, hidden, (((0,), (0,)), ((), ())), preferred_element_type=F32
    )
    grad_up = (partial_grad * act).astype(BF16)
    slope = sigmoid_gate * (1.0 + gate_wide * (1.0 - sigmoid_gate))
    grad_gate = (partial_grad * up_wide * slope).astype(BF16)
    shard_rows = lax.psum_scatter(block, "rep", scatter_dimension=0, tiled=True)
    grad_down = shard_rows.T
    row_squares = lax.psum(jnp.sum(grad_down * grad_down, axis=1), "rep")
    return (grad_gate, grad_up, grad_down, row_squares)


CHUNKS = 4
OWN, G0, G1E, G1R, G2E, G2R = (8 * i for i in range(6))
ZX, ZM, ZY, ZF, SQ_S = 48, 49, 51, 53, 55
HO_S = 58
HM_S = HO_S + CHUNKS
HF_S = HM_S + CHUNKS
C_S = HF_S + CHUNKS
N_SEM = C_S + CHUNKS


def chunk_rows(rows):
    step = -(-rows // CHUNKS)
    step = -(-step // 16) * 16
    return [(a, min(step, rows - a)) for a in range(0, rows, step)]


def kernel(gate_in, up_in, shard, w_in, gg_out, gu_out, out_out, sq_out,
           hid, G, X, Y, HO, HM, HF, CS, CR, gate, up, w, gg, gu, out, acc, SQ,
           ssem, rsem, lsem):
    rep = lax.axis_index("rep")
    fs = lax.axis_index("fs")
    tp = lax.axis_index("tp")
    tokens, wide = shard.shape
    rows = hid.shape[0]
    cols = out.shape[1]
    sub = Y.shape[2]
    half = tokens // 2
    x, y = fs % 2, fs // 2
    xq, yq, dq = y * 2 + (1 - x), (1 - y) * 2 + x, (1 - y) * 2 + (1 - x)
    me = fs * 2 + tp
    side = rep // 2
    inner = (rep == 1) | (rep == 2)
    outer = (rep == 0) | (rep == 3)
    mid = 3 - rep
    edge = side * 3
    inn = 1 + side
    far_edge = (1 - side) * 3
    far_inn = 2 - side
    partner = (rep, fs, 1 - tp)
    parts = chunk_rows(rows)
    early = range(len(parts) - 1)
    last = len(parts) - 1

    def copy(src, dst, i, dev):
        return pltpu.make_async_remote_copy(
            src_ref=src, dst_ref=dst, send_sem=ssem.at[i], recv_sem=rsem.at[i],
            device_id=dev, device_id_type=MESH)

    def at(start, size):
        return pl.ds(pl.multiple_of(start, 128), size)

    loads = [pltpu.make_async_copy(a, b, lsem.at[i])
             for i, (a, b) in enumerate([(gate_in, gate), (up_in, up), (w_in, w)])]
    for load in loads:
        load.start()

    barrier = pltpu.get_barrier_semaphore()

    def hello(dev):
        pl.semaphore_signal(barrier, inc=1, device_id=dev, device_id_type=MESH)

    for d in range(1, 4):
        hello(((rep + d) % 4, fs, tp))
    for q in (xq, yq):
        hello((rep, q, tp))
    hello(partner)
    pl.semaphore_wait(barrier, 6)

    def send_plane(base, src, view):
        copy(src, view(me), base, (rep, xq, tp)).start()
        copy(src, view(me), base + 1, (rep, yq, tp)).start()
        copy(src, view(me), base + 4, partner).start()

    def top(v):
        return v.at[pl.ds(0, half)]

    def low(v):
        return v.at[pl.ds(half, half)]

    def relay_plane(base, view):
        vx, vy, vd = view(xq * 2 + tp), view(yq * 2 + tp), view(dq * 2 + tp)
        copy(vx, vx, base, partner).wait_recv()
        copy(top(vx), top(vx), base + 2, (rep, yq, tp)).start()
        copy(vx, vx, base + 5, partner).start()
        copy(vy, vy, base + 1, partner).wait_recv()
        copy(low(vy), low(vy), base + 3, (rep, xq, tp)).start()
        copy(vy, vy, base + 6, partner).start()
        copy(top(vd), top(vd), base + 2, partner).wait_recv()
        copy(low(vd), low(vd), base + 3, partner).wait_recv()
        copy(vd, vd, base + 7, partner).start()

    def finish_plane(base, view):
        for k, q in ((4, fs), (5, xq), (6, yq), (7, dq)):
            v = view(q * 2 + 1 - tp)
            copy(v, v, base + k, partner).wait_recv()

    def sent_plane(base, view):
        v = view(me)
        for k in range(8):
            u = top(v) if k in (2, 3) else v
            copy(u, u, base + k, partner).wait_send()

    def own_view(p):
        return G.at[:, at(p * wide, wide)]

    def x_view(u):
        return lambda p: X.at[u, :, at(p * sub, sub)]

    def gcol(c):
        return G.at[:, at(c * cols + me * sub, sub)]

    x_o, m_e, m_r, f_e, f_r = (x_view(u) for u in range(5))

    def chunk(ref, c):
        a, n = parts[c]
        return ref.at[pl.ds(a, n)]

    send_plane(OWN, shard, own_view)

    loads[0].wait()
    loads[1].wait()

    def send_hidden(c):
        @pl.when(outer)
        def _():
            copy(chunk(hid, c), chunk(HO, c), HO_S + c, (inn, fs, tp)).start()

        @pl.when(inner)
        def _():
            copy(chunk(hid, c), chunk(HM, c), HM_S + c, (mid, fs, tp)).start()

    for c, (a, n) in enumerate(parts):
        r = pl.ds(a, n)
        g = gate[r, :].astype(F32)
        act = g * (1.0 / (1.0 + jnp.exp(-g)))
        hid[r, :] = (act * up[r, :].astype(F32)).astype(BF16)
        if c:
            send_hidden(c - 1)

    G[:, at(me * wide, wide)] = shard[...]
    relay_plane(OWN, own_view)
    finish_plane(OWN, own_view)

    def hidden_grads():
        loads[2].wait()
        tile = rows // 2

        @pl.loop(0, 2)
        def _(t):
            r = pl.ds(pl.multiple_of(t * tile, 16), tile)
            pg = lax.dot_general(w[r, :], G[...], (((1,), (1,)), ((), ())),
                                 preferred_element_type=F32)
            g = gate[r, :].astype(F32)
            u = up[r, :].astype(F32)
            s = 1.0 / (1.0 + jnp.exp(-g))
            gu[r, :] = (pg * (g * s)).astype(BF16)
            gg[r, :] = (pg * u * (s * (1.0 + g * (1.0 - s)))).astype(BF16)

        pltpu.make_async_copy(gg, gg_out, lsem.at[3]).start()
        pltpu.make_async_copy(gu, gu_out, lsem.at[4]).start()

    def dot(h, c, b):
        a, n = parts[c]
        return jnp.dot(h[pl.ds(a, n), :], b, preferred_element_type=F32)

    def store(c, total):
        a, n = parts[c]
        r = pl.ds(a, n)
        out[r, :] = total
        pltpu.make_async_copy(chunk(out, c), chunk(out_out, c), lsem.at[5 + c]).start()
        square = total * total
        lanes = square[:, 0:128]
        for k in range(1, cols // 128):
            lanes = lanes + square[:, k * 128:(k + 1) * 128]
        acc[r, :] = lanes

    acc[...] = jnp.zeros_like(acc)

    @pl.when(outer)
    def _():
        to = (inn, fs, tp)
        copy(gcol(far_edge), Y.at[0], ZY, to).start()
        copy(gcol(far_inn), Y.at[1], ZY + 1, to).start()
        copy(chunk(hid, last), chunk(HO, last), HO_S + last, to).start()
        copy(gcol(inn), x_o(me), ZX, to).start()
        hidden_grads()
        for c in range(len(parts)):
            a, n = parts[c]
            out[pl.ds(a, n), :] = dot(hid, c, G[:, at(rep * cols, cols)])
        for c in range(len(parts)):
            a, n = parts[c]
            copy(chunk(CS, c), chunk(CR, c), C_S + c, to).wait_recv()
            store(c, out[pl.ds(a, n), :] + CR[pl.ds(a, n), :].astype(F32))
        for c in range(len(parts)):
            copy(chunk(hid, c), chunk(HO, c), HO_S + c, to).wait_send()
        for j in range(2):
            copy(Y.at[j], Y.at[j], ZY + j, to).wait_send()
        copy(x_o(me), x_o(me), ZX, to).wait_send()

    @pl.when(inner)
    def _():
        to = (mid, fs, tp)
        back = (edge, fs, tp)

        def forward(c):
            copy(chunk(HO, c), chunk(HO, c), HO_S + c, to).wait_recv()
            copy(chunk(HO, c), chunk(HF, c), HF_S + c, to).start()

        def arrived(view, i):
            copy(view(me), view(me), i, to).wait_recv()

        copy(gcol(far_edge), m_e(me), ZM, to).start()
        copy(Y.at[0], Y.at[0], ZY, to).wait_recv()
        copy(Y.at[0], f_e(me), ZF, to).start()
        forward(0)
        arrived(m_e, ZM)
        send_plane(G1E, m_e(me), m_e)
        for c in early:
            if c:
                forward(c)
        copy(gcol(mid), m_r(me), ZM + 1, to).start()
        arrived(f_e, ZF)
        send_plane(G2E, f_e(me), f_e)
        copy(Y.at[1], Y.at[1], ZY + 1, to).wait_recv()
        copy(Y.at[1], f_r(me), ZF + 1, to).start()
        copy(chunk(hid, last), chunk(HM, last), HM_S + last, to).start()
        relay_plane(G1E, m_e)
        relay_plane(G2E, f_e)
        forward(last)
        arrived(x_o, ZX)
        send_plane(G0, x_o(me), x_o)
        finish_plane(G1E, m_e)
        finish_plane(G2E, f_e)

        def give(c):
            a, n = parts[c]
            copy(chunk(HM, c), chunk(HM, c), HM_S + c, to).wait_recv()
            copy(chunk(HF, c), chunk(HF, c), HF_S + c, to).wait_recv()
            total = dot(hid, c, G[:, at(edge * cols, cols)])
            total = total + dot(HM, c, X[1])
            total = total + dot(HF, c, X[3])
            CS[pl.ds(a, n), :] = total.astype(BF16)
            copy(chunk(CS, c), chunk(CR, c), C_S + c, back).start()

        for c in early:
            give(c)
        relay_plane(G0, x_o)
        arrived(m_r, ZM + 1)
        send_plane(G1R, m_r(me), m_r)
        arrived(f_r, ZF + 1)
        send_plane(G2R, f_r(me), f_r)
        hidden_grads()
        relay_plane(G1R, m_r)
        relay_plane(G2R, f_r)
        give(last)
        finish_plane(G0, x_o)
        finish_plane(G1R, m_r)
        finish_plane(G2R, f_r)
        for c in range(len(parts)):
            total = dot(hid, c, G[:, at(rep * cols, cols)])
            total = total + dot(HO, c, X[0])
            total = total + dot(HM, c, X[2])
            total = total + dot(HF, c, X[4])
            store(c, total)
        for j in range(2):
            copy(Y.at[j], Y.at[j], ZM + j, to).wait_send()
            copy(Y.at[j], Y.at[j], ZF + j, to).wait_send()
        for c in range(len(parts)):
            copy(chunk(HM, c), chunk(HM, c), HM_S + c, to).wait_send()
            copy(chunk(HF, c), chunk(HF, c), HF_S + c, to).wait_send()
            copy(chunk(CS, c), chunk(CS, c), C_S + c, back).wait_send()
        sent_plane(G0, x_o)
        sent_plane(G1E, m_e)
        sent_plane(G1R, m_r)
        sent_plane(G2E, f_e)
        sent_plane(G2R, f_r)

    sums = jnp.sum(acc[...].T, axis=0, keepdims=True)
    SQ[rep] = jnp.broadcast_to(sums, SQ.shape[1:])
    for d in range(1, 4):
        copy(SQ.at[rep], SQ.at[rep], SQ_S + d - 1, ((rep + d) % 4, fs, tp)).start()
    for d in range(1, 4):
        v = SQ.at[(rep + 4 - d) % 4]
        copy(v, v, SQ_S + d - 1, partner).wait_recv()
    sq_out[...] = ((SQ[0] + SQ[1]) + (SQ[2] + SQ[3]))[0:1, :rows]
    for d in range(1, 4):
        copy(SQ.at[rep], SQ.at[rep], SQ_S + d - 1, partner).wait_send()
    sent_plane(OWN, own_view)
    pltpu.make_async_copy(gg, gg_out, lsem.at[3]).wait()
    pltpu.make_async_copy(gu, gu_out, lsem.at[4]).wait()
    for c in range(len(parts)):
        pltpu.make_async_copy(chunk(out, c), chunk(out_out, c), lsem.at[5 + c]).wait()


def fused(pre_gate, pre_up, cotangent, down_weight):
    tokens, rows = pre_gate.shape
    width = down_weight.shape[1]
    reps = lax.axis_size("rep")
    plane = width // cotangent.shape[1]
    cols = width // reps
    padded = -(-rows // 128) * 128
    gate_t, up_t = pre_gate.T, pre_up.T
    vmem = pl.BlockSpec(memory_space=pltpu.VMEM)
    hbm = pl.BlockSpec(memory_space=pl.ANY)
    hid_buf = pltpu.VMEM((rows, tokens), BF16)
    gg, gu, out, squares = pl.pallas_call(
        kernel,
        out_shape=(
            jax.ShapeDtypeStruct((rows, tokens), BF16),
            jax.ShapeDtypeStruct((rows, tokens), BF16),
            jax.ShapeDtypeStruct((rows, cols), F32),
            jax.ShapeDtypeStruct((1, rows), F32),
        ),
        in_specs=[hbm, hbm, vmem, hbm],
        out_specs=(hbm, hbm, hbm, vmem),
        scratch_shapes=[
            hid_buf,
            pltpu.VMEM((tokens, width), BF16),
            pltpu.VMEM((5, tokens, cols), BF16),
            pltpu.VMEM((2, tokens, cols // plane), BF16),
            hid_buf, hid_buf, hid_buf,
            pltpu.VMEM((rows, cols), BF16),
            pltpu.VMEM((rows, cols), BF16),
            hid_buf, hid_buf,
            pltpu.VMEM((rows, width), BF16),
            hid_buf, hid_buf,
            pltpu.VMEM((rows, cols), F32),
            pltpu.VMEM((padded, 128), F32),
            pltpu.VMEM((4, 8, padded), F32),
            pltpu.SemaphoreType.DMA((N_SEM,)),
            pltpu.SemaphoreType.DMA((N_SEM,)),
            pltpu.SemaphoreType.DMA((5 + CHUNKS,)),
        ],
        compiler_params=pltpu.CompilerParams(
            collective_id=0, has_side_effects=True, vmem_limit_bytes=67043328),
    )(gate_t, up_t, cotangent, down_weight)
    return gg.T, gu.T, out, squares.reshape(rows)


def solution(mesh):
    placed = (
        P("rep", ("fs", "tp")),
        P("rep", ("fs", "tp")),
        P("rep", ("fs", "tp")),
        P(("fs", "tp"), None),
    )
    shape = dict(mesh.shape)
    fits = shape["rep"] // 2 == 2 and shape["fs"] // 2 == 2 and shape["tp"] == 2
    return jax.shard_map(
        fused if fits else local,
        mesh=mesh,
        in_specs=placed,
        out_specs=(
            P("rep", ("fs", "tp")),
            P("rep", ("fs", "tp")),
            P(("fs", "tp"), "rep"),
            P(("fs", "tp")),
        ),
        check_vma=False,
    )
```
